32 devices in a mesh: ep: 16 (over z, y, x), tp: 2 (over core).
Axes of the slice: x: 2, y: 2, z: 4, core: 2. Of those that a mesh axis runs over, the one named last changes fastest.
Arguments:
- tokens: bfloat16 [192, 2048], P('ep', 'tp'), may hold values from -21 to 21
- norm_gain: bfloat16 [2048], P('tp'), may hold values from 0.099609375 to 1.8984375
- expert_ids: int32 [192, 8], P('ep'), may hold values from 0 to 31, all different within a row; in each aligned block of 12 rows (0 to 11, 12 to 23, ...) at most 5 rows name the same one
- route_gate: float32 [192, 8], P('ep'), may hold values from 0.05 to 1
- w_gate: bfloat16 [32, 2048, 512], P('ep', None, 'tp'), may hold values from -0.125 to 0.125
- w_up: bfloat16 [32, 2048, 512], P('ep', None, 'tp'), may hold values from -0.125 to 0.125
- w_down: bfloat16 [32, 512, 2048], P('ep', 'tp'), may hold values from -0.25 to 0.25
- shared_gate: bfloat16 [2048, 512], P(None, 'tp'), may hold values from -0.125 to 0.125
- shared_up: bfloat16 [2048, 512], P(None, 'tp'), may hold values from -0.125 to 0.125
- shared_down: bfloat16 [512, 2048], P('tp'), may hold values from -0.25 to 0.25
Outputs:
- mixed: bfloat16 [192, 2048], P('ep', 'tp')
The draws below stay inside these ranges and needn't reach their ends.
Inputs may be any that keep to these rules, and one draw needn't show every extreme that they name: `expert_ids`: each row names 8 different experts; among the 12 rows of one device no expert is named more than once.
All inputs are finite; a program needn't handle non-finite values.
Results may differ from the reference program's by a relative error of at most 0.012.
Values may be sent and summed in bfloat16 or wider, within the bound.
A program may use at most 64 MiB of HBM per device.

```python
import math
import jax
import jax.numpy as jnp
import numpy as np
from jax import lax

D = 2048
FE = 512
FS = 512
TOP = 8
TOK_DEV = 12
EXPERTS = 32
TOKENS = 192
CAP = 5
N_EP = 16
N_TP = 2


def draw_tokens(key, part):
    first_key, second_key, third_key = jax.random.split(jax.random.fold_in(key, 11), 3)
    chosen = jax.random.randint(third_key, (), 0, 2)
    columns = jnp.arange(D, dtype=jnp.int32)
    upper = (columns < D // 2).astype(jnp.int32) == chosen
    column_scale = jnp.where(upper, 3.0, 1.0).astype(jnp.float32)
    plain_values = jnp.clip(jax.random.normal(first_key, (TOKENS, D), jnp.float32), -4.0, 4.0)
    row_scale = jnp.exp(jax.random.uniform(second_key, (TOKENS, 1), jnp.float32, -0.5, 0.5))
    return (plain_values * row_scale * column_scale[None, :]).astype(jnp.bfloat16)


def steps_of(own_key, dims, shards, smallest, top_value):
    level = 1.0
    for dim, blocks in shards:
        heights = jax.random.uniform(jax.random.fold_in(jax.random.fold_in(own_key, 6), dim), (blocks,), jnp.float32, smallest / len(shards), top_value / len(shards))
        level = level * jnp.repeat(jnp.exp(heights), dims[dim] // blocks).reshape((-1,) + (1,) * (len(dims) - 1 - dim))
    return level


def assign_block(own_key, own, number, rows, number_of, top, bound, slope):
    order = jax.random.permutation(own_key, number_of)
    heavy_load, ordinary = portions_of(number_of, rows * top, bound, slope, True), portions_of(number_of, rows * top, bound, slope, False)
    places = jnp.arange(number_of)

    def named(sizes, rotation):
        used = int((sizes > 0).sum())
        fixed = max(1, used // 4)
        moved = fixed + (places - fixed + rotation * (used - fixed)) % max(1, number_of - fixed)
        return jnp.zeros((number_of,), jnp.int32).at[order[jnp.where(places < fixed, places, moved)]].set(jnp.asarray(sizes, jnp.int32))

    sizes = jnp.where(number % 4 == 0, named(heavy_load, number // 4), named(ordinary, number - number // 4 - 1))
    mixed = jax.random.permutation(jax.random.fold_in(own, 3), number_of)
    giver, sink = mixed[0:number_of // 2 * 2:2], mixed[1:number_of // 2 * 2:2]
    room = jnp.minimum(sizes[giver] - 1, bound - sizes[sink]) // 2
    room = jnp.where((giver == order[0]) | (sink == order[0]) | (sizes[sink] == 0), 0, jnp.maximum(room, 0))
    moved = jax.random.randint(jax.random.fold_in(own, 4), (number_of // 2,), 0, 1 << 20) % (room + 1)
    sizes = sizes.at[giver].add(-moved).at[sink].add(moved)
    members = jnp.searchsorted(jnp.cumsum(sizes), jnp.arange(rows * top), side="right").astype(jnp.int32)
    listing = members.reshape(top, rows).T
    listing = listing[jax.random.permutation(jax.random.fold_in(own, 1), rows)]
    rotation = jax.random.randint(jax.random.fold_in(own, 2), (rows, 1), 0, top)
    return jnp.take_along_axis(listing, (jnp.arange(top)[None, :] + rotation) % top, axis=1)


def portions_of(amount, total, bound, skew, full):
    weights = [(1 << 20) // math.isqrt(standing ** skew) + 1 for standing in range(1, amount + 1)]
    largest = bound if full else min(bound, max(-(-total // amount), total * weights[0] // sum(weights)))
    least = 1 if total - largest >= amount - 1 else 0
    given, rest = [largest] + [least] * (amount - 1), total - largest - least * (amount - 1)
    while rest > 0:
        candidates = [i for i in range(1, amount) if given[i] < largest] or [i for i in range(1, amount) if given[i] < bound]
        pool, left = sum([weights[i] for i in candidates]), rest
        for i in candidates:
            more = min(bound - given[i], max(1, left * weights[i] // pool), rest)
            given[i] = given[i] + more
            rest = rest - more
    return np.array(given)


def centred(own_key, extent, scale, reach, shards=(), kind=jnp.bfloat16):
    result = jax.random.normal(own_key, extent, jnp.float32) * scale
    if len(shards) > 0:
        result = steps_of(own_key, extent, shards, -0.22, 0.18) * result
    return jnp.clip(result, min=-reach, max=reach).astype(kind)


def setup_inputs(seed: int = 0) -> dict:
    key_list = jax.random.split(jax.random.key(seed), 11)
    tokens = draw_tokens(jax.random.fold_in(key_list[10], 71), 0)
    norm_gain = jnp.clip(1.0 + 0.18 * jax.random.normal(key_list[1], (D,), jnp.float32), 0.099609375, 1.8984375).astype(jnp.bfloat16)
    expert_ids_keys = jax.random.split(jax.random.fold_in(key_list[2], 1), TOKENS // TOK_DEV)
    expert_ids_turns = jax.random.permutation(jax.random.fold_in(key_list[2], 3), TOKENS // TOK_DEV)
    expert_ids = jax.vmap(lambda own, number: assign_block(jax.random.fold_in(key_list[2], 2), own, number, TOK_DEV, EXPERTS, TOP, CAP, 2))(expert_ids_keys, expert_ids_turns).reshape((TOKENS, TOP))
    route_gate = jnp.clip(jnp.exp(math.log(1.0) - 2.9957323 * jax.random.uniform(key_list[3], (TOKENS, TOP), jnp.float32) ** steps_of(key_list[3], (TOKENS, TOP), ((0, 16),), -0.2, 0.2)), 0.05, 1.0)
    w_gate = centred(key_list[4], (EXPERTS, D, FE), D ** -0.5, 0.125, ((0, 16), (2, 2)))
    w_up = centred(key_list[5], (EXPERTS, D, FE), D ** -0.5, 0.125, ((0, 16), (2, 2)))
    w_down = centred(key_list[6], (EXPERTS, FE, D), FE ** -0.5, 0.25, ((0, 16), (1, 2)))
    shared_gate = centred(key_list[7], (D, FS), D ** -0.5, 0.125, ((1, 2),))
    shared_up = centred(key_list[8], (D, FS), D ** -0.5, 0.125, ((1, 2),))
    shared_down = centred(key_list[9], (FS, D), FS ** -0.5, 0.25, ((0, 2),))
    return dict(tokens=tokens, norm_gain=norm_gain, expert_ids=expert_ids, route_gate=route_gate, w_gate=w_gate, w_up=w_up, w_down=w_down, shared_gate=shared_gate, shared_up=shared_up, shared_down=shared_down)


eps = 1e-06
routed_scale = 2.5

def reference(tokens, norm_gain, expert_ids, route_gate, w_gate, w_up, w_down, shared_gate, shared_up, shared_down):
    values = tokens.astype(jnp.float32)
    mean_sq = lax.optimization_barrier(jnp.mean(values * values, axis=-1, keepdims=True))
    normed = (values * lax.rsqrt(mean_sq + eps) * norm_gain.astype(jnp.float32)).astype(jnp.bfloat16)
    weight = route_gate / lax.optimization_barrier(jnp.sum(route_gate, axis=-1, keepdims=True)) * routed_scale
    pairs = TOK_DEV * TOP
    block_ids = expert_ids.reshape(N_EP, pairs)
    position = jnp.arange(pairs, dtype=jnp.int32)
    equal_ids = block_ids[:, :, None] == block_ids[:, None, :]
    earlier = position[None, :] < position[:, None]
    ranking = lax.optimization_barrier(jnp.sum(equal_ids & earlier[None], axis=-1)).astype(jnp.int32)
    per_expert = N_EP * CAP
    slot = block_ids * per_expert + jnp.arange(N_EP, dtype=jnp.int32)[:, None] * CAP + ranking
    slot = slot.reshape(TOKENS * TOP).astype(jnp.int32)
    owner = (jnp.arange(TOKENS * TOP, dtype=jnp.int32) // TOP).astype(jnp.int32)
    table = jnp.full((EXPERTS * per_expert,), TOKENS, jnp.int32).at[slot].set(owner)
    padded_rows = jnp.concatenate([normed, jnp.zeros((1, D), jnp.bfloat16)], axis=0)

    def one_expert(args):
        gate_w, up_w, down_w, rows = args
        inputs = padded_rows[rows]
        gate_value = jnp.dot(inputs, gate_w, preferred_element_type=jnp.float32)
        up_value = jnp.dot(inputs, up_w, preferred_element_type=jnp.float32)
        hidden = (jax.nn.silu(gate_value) * up_value).astype(jnp.bfloat16)
        pieces = hidden.reshape(per_expert, N_TP, FE // N_TP).astype(jnp.float32)
        down_pieces = down_w.reshape(N_TP, FE // N_TP, D).astype(jnp.float32)
        parts = jnp.einsum('rpf,pfd->prd', pieces, down_pieces).astype(jnp.bfloat16)
        return lax.optimization_barrier(jnp.sum(parts.astype(jnp.float32), axis=0)).astype(jnp.bfloat16)
    outputs = lax.map(one_expert, (w_gate, w_up, w_down, table.reshape(EXPERTS, per_expert)))
    picked = outputs.reshape(EXPERTS * per_expert, D)[slot].reshape(TOKENS, TOP, D)
    routed = lax.optimization_barrier(jnp.sum(picked.astype(jnp.float32) * weight[:, :, None], axis=1))
    gate_value = jnp.dot(normed, shared_gate, preferred_element_type=jnp.float32)
    up_value = jnp.dot(normed, shared_up, preferred_element_type=jnp.float32)
    shared_hidden = (jax.nn.silu(gate_value) * up_value).astype(jnp.bfloat16)
    shared = jnp.dot(shared_hidden, shared_down, preferred_element_type=jnp.float32)
    return (routed + shared).astype(jnp.bfloat16)
```

```python
import functools
import math

import jax
import jax.numpy as jnp
from jax import lax
from jax.experimental import pallas as pl
from jax.experimental.pallas import tpu as pltpu
from jax.sharding import PartitionSpec as P

eps = 1e-06
routed_scale = 2.5
MESH = pl.DeviceIdType.MESH
f32 = jnp.float32
bf16 = jnp.bfloat16


def kernel(
    n_ep, plane, rows, chunk,
    tok, gain, ids, gates, wg_h, wu_h, wd_h, sg_h, su_h, sd_h,
    out,
    g, wg, wu, wd, sg, su, hid, ysend, yrecv, yown, sums, r1, tsum, r2,
    wsem, zs, zr, ps, pr, ds, dr, ys, yr, rs, rr, bs, br,
):
    nz = n_ep // plane
    e = lax.axis_index("ep")
    c = lax.axis_index("tp")
    other = 1 - c
    z, q = e // plane, e % plane
    tok_dev, half = tok.shape
    exp_dev, feats, hidden = wg_h.shape
    experts = exp_dev * n_ep
    width = g.shape[3]
    tile = ysend.shape[2]
    tiles = half // tile
    chunks = n_ep * rows // chunk
    per = chunk // rows

    def ep_of(zi, qi):
        return zi * plane + qi

    z_others = [(z + d) % nz for d in range(1, nz)]
    q_others = [(q + d) % plane for d in range(1, plane)]

    barrier = pltpu.get_barrier_semaphore()
    for zi in z_others:
        pl.semaphore_signal(barrier, inc=1, device_id={"ep": ep_of(zi, q)}, device_id_type=MESH)
    for qi in q_others:
        pl.semaphore_signal(barrier, inc=1, device_id={"ep": ep_of(z, qi)}, device_id_type=MESH)
    pl.semaphore_signal(barrier, inc=1, device_id={"tp": other}, device_id_type=MESH)

    loads = [
        pltpu.make_async_copy(sg_h, sg, wsem.at[0]),
        pltpu.make_async_copy(su_h, su, wsem.at[1]),
        pltpu.make_async_copy(wg_h, wg, wsem.at[2]),
        pltpu.make_async_copy(wu_h, wu, wsem.at[3]),
        pltpu.make_async_copy(sd_h, wd.at[pl.ds(exp_dev * hidden, hidden)], wsem.at[4]),
    ]
    for j in range(exp_dev):
        loads.append(
            pltpu.make_async_copy(wd_h.at[j], wd.at[pl.ds(j * hidden, hidden)], wsem.at[5 + j])
        )
    for load in loads:
        load.start()

    values = tok[...].astype(f32)
    squares = jnp.sum(values * values, axis=-1, keepdims=True)
    weight = gates[...] / jnp.sum(gates[...], axis=-1, keepdims=True) * routed_scale
    lane = lax.broadcasted_iota(jnp.int32, (tok_dev, width - half), 1)
    dense = jnp.zeros((tok_dev, width - half), f32)
    chosen = ids[...]
    for k in range(chosen.shape[1]):
        dense += jnp.where(lane == chosen[:, k : k + 1], weight[:, k : k + 1], 0.0)
    dense_hi = dense.astype(bf16).astype(f32)
    extra = jnp.where(c == 0, dense_hi, dense - dense_hi)
    sq_a = squares.astype(bf16).astype(f32)
    sq_b = (squares - sq_a).astype(bf16).astype(f32)
    sq_c = squares - sq_a - sq_b
    extra = jnp.where(lane == experts, sq_a, extra)
    extra = jnp.where(lane == experts + 1, sq_b, extra)
    extra = jnp.where(lane == experts + 2, sq_c, extra)
    g[c, e] = jnp.zeros((rows, width), bf16)
    g[c, e, :tok_dev, :half] = (values * gain[...].astype(f32)).astype(bf16)
    g[c, e, :tok_dev, half:] = extra.astype(bf16)
    hid[:, exp_dev * hidden :] = jnp.zeros((hid.shape[0], hidden), bf16)

    pl.semaphore_wait(barrier, (nz - 1) + (plane - 1) + 1)

    def z_copy(zi):
        return pltpu.make_async_remote_copy(
            src_ref=g.at[c, e], dst_ref=g.at[c, e], send_sem=zs.at[zi], recv_sem=zr.at[z],
            device_id={"ep": ep_of(zi, q)}, device_id_type=MESH)

    def z_arrival(zi):
        piece = g.at[c, ep_of(zi, q)]
        return pltpu.make_async_remote_copy(
            src_ref=piece, dst_ref=piece, send_sem=zs.at[zi], recv_sem=zr.at[zi],
            device_id={"ep": ep_of(zi, q)}, device_id_type=MESH)

    def plane_copy(zi, qi):
        piece = g.at[c, ep_of(zi, q)]
        return pltpu.make_async_remote_copy(
            src_ref=piece, dst_ref=piece, send_sem=ps.at[qi, zi], recv_sem=pr.at[q, zi],
            device_id={"ep": ep_of(z, qi)}, device_id_type=MESH)

    def plane_arrival(zi, qi):
        piece = g.at[c, ep_of(zi, qi)]
        return pltpu.make_async_remote_copy(
            src_ref=piece, dst_ref=piece, send_sem=ps.at[qi, zi], recv_sem=pr.at[qi, zi],
            device_id={"ep": ep_of(z, qi)}, device_id_type=MESH)

    def partner_copy(ei):
        piece = g.at[c, ei]
        return pltpu.make_async_remote_copy(
            src_ref=piece, dst_ref=piece, send_sem=ds.at[ei], recv_sem=dr.at[ei],
            device_id={"tp": other}, device_id_type=MESH)

    def partner_arrival(ei):
        piece = g.at[other, ei]
        return pltpu.make_async_remote_copy(
            src_ref=piece, dst_ref=piece, send_sem=ds.at[ei], recv_sem=dr.at[ei],
            device_id={"tp": other}, device_id_type=MESH)

    for zi in z_others:
        z_copy(zi).start()
    for qi in q_others:
        plane_copy(z, qi).start()
    partner_copy(e).start()

    for zi in z_others:
        z_arrival(zi).wait_recv()
        for qi in q_others:
            plane_copy(zi, qi).start()
        partner_copy(ep_of(zi, q)).start()

    def row_scale(extras):
        lanes = lax.broadcasted_iota(jnp.int32, extras.shape, 1)
        inside = (lanes >= experts) & (lanes < experts + 3)
        total = jnp.sum(jnp.where(inside, extras, 0.0), axis=-1, keepdims=True)
        return lax.rsqrt(total / feats + eps)

    def gated(gate_value, up_value, scale):
        gate_value, up_value = gate_value * scale, up_value * scale
        return gate_value / (1.0 + jnp.exp(-gate_value)) * up_value

    partner_arrival(e).wait_recv()
    loads[0].wait()
    loads[1].wait()
    own_0, own_1 = g[0, e], g[1, e]
    scale = row_scale(own_0[:, half:].astype(f32) + own_1[:, half:].astype(f32))
    gate_value = jnp.dot(own_0[:, :half], sg[:half], preferred_element_type=f32)
    gate_value += jnp.dot(own_1[:, :half], sg[half:], preferred_element_type=f32)
    up_value = jnp.dot(own_0[:, :half], su[:half], preferred_element_type=f32)
    up_value += jnp.dot(own_1[:, :half], su[half:], preferred_element_type=f32)
    hid[pl.ds(pl.multiple_of(e * rows, rows), rows), exp_dev * hidden :] = gated(
        gate_value, up_value, scale).astype(bf16)

    for zi in [z] + z_others:
        for qi in q_others:
            plane_arrival(zi, qi).wait_recv()
            partner_copy(ep_of(zi, qi)).start()
    for zi in z_others:
        partner_arrival(ep_of(zi, q)).wait_recv()
    for zi in [z] + z_others:
        for qi in q_others:
            partner_arrival(ep_of(zi, qi)).wait_recv()
    for load in loads[2:]:
        load.wait()

    def partner_tile(m, n):
        return pltpu.make_async_remote_copy(
            src_ref=ysend.at[n, pl.ds(m * chunk, chunk)], dst_ref=yrecv.at[n, pl.ds(m * chunk, chunk)],
            send_sem=ys.at[m, n], recv_sem=yr.at[m, n],
            device_id={"tp": other}, device_id_type=MESH)

    def compute(m, carry):
        first = pl.multiple_of(m * chunk, chunk)
        block_0 = g[0, pl.ds(m * per, per)].reshape(chunk, width)
        block_1 = g[1, pl.ds(m * per, per)].reshape(chunk, width)
        x_0, x_1 = block_0[:, :half], block_1[:, :half]
        extras = block_0[:, half:].astype(f32) + block_1[:, half:].astype(f32)
        scale = row_scale(extras)
        lanes = lax.broadcasted_iota(jnp.int32, extras.shape, 1)
        for j in range(exp_dev):
            weights = jnp.sum(jnp.where(lanes == e * exp_dev + j, extras, 0.0), axis=-1, keepdims=True)
            gate_value = jnp.dot(x_0, wg[j, :half], preferred_element_type=f32)
            gate_value += jnp.dot(x_1, wg[j, half:], preferred_element_type=f32)
            up_value = jnp.dot(x_0, wu[j, :half], preferred_element_type=f32)
            up_value += jnp.dot(x_1, wu[j, half:], preferred_element_type=f32)
            hid[pl.ds(first, chunk), j * hidden : (j + 1) * hidden] = (
                gated(gate_value, up_value, scale) * weights).astype(bf16)
        h = hid[pl.ds(first, chunk)]
        for n in range(tiles):
            columns = pl.ds(pl.multiple_of(other * half + n * tile, tile), tile)
            ysend[n, pl.ds(first, chunk)] = jnp.dot(
                h, wd[:, columns], preferred_element_type=f32).astype(bf16)
            partner_tile(m, n).start()
        for n in range(tiles):
            columns = pl.ds(pl.multiple_of(c * half + n * tile, tile), tile)
            yown[n, pl.ds(first, chunk)] = jnp.dot(h, wd[:, columns], preferred_element_type=f32)
        return carry

    lax.fori_loop(0, chunks, compute, 0)

    def add_partner(m, carry):
        first = pl.multiple_of(m * chunk, chunk)
        for n in range(tiles):
            partner_tile(m, n).wait_recv()
            total = yown[n, pl.ds(first, chunk)] + yrecv[n, pl.ds(first, chunk)].astype(f32)
            sums[pl.ds(m * per, per), :, n * tile : (n + 1) * tile] = total.astype(bf16).reshape(
                per, rows, tile)
        return carry

    lax.fori_loop(0, chunks, add_partner, 0)

    def plane_sum(zi, qi):
        return pltpu.make_async_remote_copy(
            src_ref=sums.at[ep_of(zi, qi)], dst_ref=r1.at[q, zi], send_sem=rs.at[qi, zi],
            recv_sem=rr.at[q, zi], device_id={"ep": ep_of(z, qi)}, device_id_type=MESH)

    def plane_sum_arrival(zi, qi):
        return pltpu.make_async_remote_copy(
            src_ref=sums.at[ep_of(zi, qi)], dst_ref=r1.at[qi, zi], send_sem=rs.at[qi, zi],
            recv_sem=rr.at[qi, zi], device_id={"ep": ep_of(z, qi)}, device_id_type=MESH)

    def z_sum(zi):
        return pltpu.make_async_remote_copy(
            src_ref=tsum.at[zi], dst_ref=r2.at[z], send_sem=bs.at[zi], recv_sem=br.at[z],
            device_id={"ep": ep_of(zi, q)}, device_id_type=MESH)

    def z_sum_arrival(zi):
        return pltpu.make_async_remote_copy(
            src_ref=tsum.at[zi], dst_ref=r2.at[zi], send_sem=bs.at[zi], recv_sem=br.at[zi],
            device_id={"ep": ep_of(zi, q)}, device_id_type=MESH)

    for zi in z_others + [z]:
        for qi in q_others:
            plane_sum(zi, qi).start()
    total = None
    for zi in z_others + [z]:
        total = sums[ep_of(zi, q)].astype(f32)
        for qi in q_others:
            plane_sum_arrival(zi, qi).wait_recv()
            total += r1[qi, zi].astype(f32)
        if zi is not z:
            tsum[zi] = total.astype(bf16)
            z_sum(zi).start()
    for zi in z_others:
        z_sum_arrival(zi).wait_recv()
        total += r2[zi].astype(f32)
    out[...] = total[:tok_dev].astype(bf16)

    for zi in z_others:
        z_copy(zi).wait_send()
        z_sum(zi).wait_send()
    for zi in [z] + z_others:
        for qi in q_others:
            plane_copy(zi, qi).wait_send()
            plane_sum(zi, qi).wait_send()
            partner_copy(ep_of(zi, qi)).wait_send()
        partner_copy(ep_of(zi, q)).wait_send()

    def finish(m, carry):
        for n in range(tiles):
            partner_tile(m, n).wait_send()
        return carry

    lax.fori_loop(0, chunks, finish, 0)


def local(tokens, norm_gain, expert_ids, route_gate, w_gate, w_up, w_down, shared_gate, shared_up, shared_down):
    n_ep = lax.axis_size("ep")
    tok_dev, half = tokens.shape
    exp_dev, feats, hidden = w_gate.shape
    plane = math.gcd(n_ep, 2 ** (int(math.log2(n_ep)) // 2))
    nz = n_ep // plane
    rows = -(-tok_dev // 16) * 16
    total_rows = n_ep * rows
    chunk = rows * math.gcd(n_ep, max(1, 256 // rows))
    chunks = total_rows // chunk
    tile = min(512, half)
    tiles = half // tile
    width = half + -(-(exp_dev * n_ep + 3) // 128) * 128
    vmem = pl.BlockSpec(memory_space=pltpu.VMEM)
    anywhere = pl.BlockSpec(memory_space=pl.ANY)
    dma = pltpu.SemaphoreType.DMA
    k_rows = (exp_dev + 1) * hidden
    return pl.pallas_call(
        functools.partial(kernel, n_ep, plane, rows, chunk),
        out_shape=jax.ShapeDtypeStruct((tok_dev, half), bf16),
        in_specs=[vmem] * 4 + [anywhere] * 6,
        out_specs=vmem,
        scratch_shapes=[
            pltpu.VMEM((2, n_ep, rows, width), bf16),
            pltpu.VMEM(w_gate.shape, bf16),
            pltpu.VMEM(w_up.shape, bf16),
            pltpu.VMEM((k_rows, feats), bf16),
            pltpu.VMEM(shared_gate.shape, bf16),
            pltpu.VMEM(shared_up.shape, bf16),
            pltpu.VMEM((total_rows, k_rows), bf16),
            pltpu.VMEM((tiles, total_rows, tile), bf16),
            pltpu.VMEM((tiles, total_rows, tile), bf16),
            pltpu.VMEM((tiles, total_rows, tile), f32),
            pltpu.VMEM((n_ep, rows, half), bf16),
            pltpu.VMEM((plane, nz, rows, half), bf16),
            pltpu.VMEM((nz, rows, half), bf16),
            pltpu.VMEM((nz, rows, half), bf16),
            dma((5 + exp_dev,)),
            dma((nz,)), dma((nz,)),
            dma((plane, nz)), dma((plane, nz)),
            dma((n_ep,)), dma((n_ep,)),
            dma((chunks, tiles)), dma((chunks, tiles)),
            dma((plane, nz)), dma((plane, nz)),
            dma((nz,)), dma((nz,)),
        ],
        compiler_params=pltpu.CompilerParams(
            collective_id=0, has_side_effects=True, vmem_limit_bytes=64 * 1024 * 1024 - 131072),
    )(tokens, norm_gain.reshape(1, half), expert_ids, route_gate, w_gate, w_up, w_down,
      shared_gate, shared_up, shared_down)


def solution(mesh):
    in_specs = (
        P("ep", "tp"),
        P("tp"),
        P("ep", None),
        P("ep", None),
        P("ep", None, "tp"),
        P("ep", None, "tp"),
        P("ep", "tp", None),
        P(None, "tp"),
        P(None, "tp"),
        P("tp", None),
    )
    out_specs = P("ep", "tp")
    return jax.shard_map(local, mesh=mesh, in_specs=in_specs, out_specs=out_specs, check_vma=False)
```
